512 devices in a mesh: sp: 64 (over z, y), tp: 8 (over x, core).
Axes of the slice: x: 4, y: 4, z: 16, core: 2. Of those that a mesh axis runs over, the one named last changes fastest.
Arguments:
- tokens: bfloat16 [2, 16384, 2048], P(None, 'sp'), may hold values from -6 to 6
- key_weight: bfloat16 [2048, 2048], P(None, 'tp'), may hold values from -0.125 to 0.125
- value_weight: bfloat16 [2048, 2048], P(None, 'tp'), may hold values from -0.125 to 0.125
- cum_gate: float32 [2, 16384, 32], P(None, 'sp', 'tp'), may hold values from -1968.2 to 0, as said below
- new_input: bfloat16 [2, 2048], replicated, may hold values from -6 to 6
- new_query: bfloat16 [2, 2048], P(None, 'tp'), may hold values from -360 to 360
- new_gate: float32 [2, 32], P(None, 'tp'), may hold values from -1968.2 to 0
- out_weight: bfloat16 [2048, 2048], P('tp', 'sp'), may hold values from -0.75 to 0.75
Outputs:
- key_cache: bfloat16 [2, 64, 256, 2048], P(None, 'sp', None, 'tp')
- value_cache: bfloat16 [2, 64, 256, 2048], P(None, 'sp', None, 'tp')
- gate_cache: float32 [2, 64, 256, 32], P(None, 'sp', None, 'tp')
- mixed: bfloat16 [2, 2048], P(None, 'sp')
The draws below stay inside these ranges and needn't reach their ends.
Inputs may be any that keep to these rules, and one draw needn't show every extreme that they name: For each sequence and head cum_gate does not rise along positions, and new_gate lies at or below the value at the last cached position.
All inputs are finite; a program needn't handle non-finite values.
Results may differ from the reference program's by a relative error of at most 0.015.
Values may be sent and summed in bfloat16 or wider, within the bound.
A program may use at most 64 MiB of HBM per device.

```python
import math
import jax
import jax.numpy as jnp
from jax import lax

D = 2048
ATTENTION_HEADS = 32
HEAD_DIM = 64
BATCH_SEQUENCES = 2
SPAN = 256
CACHED_LENGTH = 16384
N_SP = 64
N_TP = 8


def gate_logs(key):
    head_order = jax.random.permutation(jax.random.fold_in(key, 1), ATTENTION_HEADS)
    lagging_heads = head_order < ATTENTION_HEADS // 2
    fast_rate = jnp.exp(jax.random.uniform(jax.random.fold_in(key, 2), (ATTENTION_HEADS,), jnp.float32, math.log(0.01), math.log(1.0 / 30.0)))
    slow_rate = jax.random.uniform(jax.random.fold_in(key, 3), (ATTENTION_HEADS,), jnp.float32, 0.2, 0.6) / (CACHED_LENGTH + 1)
    decay_rate = jnp.where(lagging_heads, slow_rate, fast_rate)
    block_count = CACHED_LENGTH // SPAN
    decay_factor = jnp.exp(jax.random.uniform(jax.random.fold_in(key, 4), (BATCH_SEQUENCES, block_count, 1, ATTENTION_HEADS), jnp.float32, math.log(0.5), math.log(2.0)))
    decay_factor = jnp.broadcast_to(decay_factor, (BATCH_SEQUENCES, block_count, SPAN, ATTENTION_HEADS)).reshape(BATCH_SEQUENCES, CACHED_LENGTH, ATTENTION_HEADS)
    decay_factor = jnp.concatenate([decay_factor, jnp.ones((BATCH_SEQUENCES, 1, ATTENTION_HEADS), jnp.float32)], axis=1)
    random_jitter = jax.random.uniform(jax.random.fold_in(key, 5), (BATCH_SEQUENCES, CACHED_LENGTH + 1, ATTENTION_HEADS), jnp.float32, 0.3, 1.7)
    spike_positions = jax.random.randint(jax.random.fold_in(key, 6), (BATCH_SEQUENCES, 2, ATTENTION_HEADS), 0, CACHED_LENGTH + 1)
    position_index = jnp.arange(CACHED_LENGTH + 1, dtype=jnp.int32)
    spike_count = jnp.sum((position_index[None, :, None, None] == spike_positions[:, None, :, :]).astype(jnp.float32), axis=2)
    spike_height = jax.random.uniform(jax.random.fold_in(key, 7), (BATCH_SEQUENCES, CACHED_LENGTH + 1, ATTENTION_HEADS), jnp.float32, 0.22, 0.69)
    forget_logits = -decay_rate * decay_factor * random_jitter - spike_count * spike_height * lagging_heads.astype(jnp.float32)
    return jnp.cumsum(forget_logits, axis=1)


def draw_cum_gate(key, part):
    return gate_logs(key)[:, :CACHED_LENGTH, :]


def draw_new_gate(key, part):
    return gate_logs(key)[:, CACHED_LENGTH, :]


def draw_new_query(key, part):
    query_base = jax.random.truncated_normal(jax.random.fold_in(key, 21), -6.0, 6.0, (BATCH_SEQUENCES, D), jnp.float32)
    return query_base.astype(jnp.bfloat16)


def level_of(key, extent, cuts, low, high):
    gain = 1.0
    for axis_at, blocks in cuts:
        draws = jax.random.uniform(jax.random.fold_in(jax.random.fold_in(key, 6), axis_at), (blocks,), jnp.float32, low / len(cuts), high / len(cuts))
        gain = gain * jnp.repeat(jnp.exp(draws), extent[axis_at] // blocks).reshape((-1,) + (1,) * (len(extent) - 1 - axis_at))
    return gain


def scatter_about(own_key, shape, scale, limit, cuts=(), held_as=jnp.bfloat16):
    drawn = scale * jax.random.normal(own_key, shape, jnp.float32)
    if cuts:
        drawn = drawn * level_of(own_key, shape, cuts, -0.22, 0.18)
    return jnp.clip(drawn, -limit, limit).astype(held_as)


def setup_inputs(seed: int = 0) -> dict:
    streams_of = jax.random.split(jax.random.key(seed), 9)
    return {
        "tokens": scatter_about(streams_of[0], (BATCH_SEQUENCES, CACHED_LENGTH, D), 1.0, 6.0, ((1, 64),)),
        "key_weight": scatter_about(streams_of[1], (D, D), D ** -0.5, 0.125, ((1, 8),)),
        "value_weight": scatter_about(streams_of[2], (D, D), D ** -0.5, 0.125, ((1, 8),)),
        "cum_gate": draw_cum_gate(jax.random.fold_in(streams_of[8], 71), 0),
        "new_input": scatter_about(streams_of[4], (BATCH_SEQUENCES, D), 1.0, 6.0),
        "new_query": draw_new_query(jax.random.fold_in(streams_of[8], 71), 0),
        "new_gate": draw_new_gate(jax.random.fold_in(streams_of[8], 71), 0),
        "out_weight": scatter_about(streams_of[7], (D, D), HEAD_DIM ** -0.5, 0.75, ((0, 8), (1, 64))),
    }


def cyclic(rows):
    shaped = rows.reshape(rows.shape[0], SPAN, N_SP, rows.shape[2])
    return jnp.transpose(shaped, (0, 2, 1, 3))


def read_one(inputs):
    key_rows, value_rows, gate_rows, query_row, gate_now, key_now, value_now = inputs
    score_scale = HEAD_DIM ** -0.5
    key_heads = key_rows.reshape(N_SP, SPAN, ATTENTION_HEADS, HEAD_DIM).astype(jnp.float32)
    value_heads = value_rows.reshape(N_SP, SPAN, ATTENTION_HEADS, HEAD_DIM).astype(jnp.float32)
    query_heads = query_row.reshape(ATTENTION_HEADS, HEAD_DIM).astype(jnp.float32)
    scores = jnp.einsum("hd,rlhd->hrl", query_heads, key_heads) * score_scale
    scores = scores + gate_now[:, None, None] - jnp.transpose(gate_rows, (2, 0, 1))
    class_top = jnp.max(scores, axis=2)
    expo = jnp.exp(scores - class_top[:, :, None])
    class_total = jnp.sum(expo, axis=2)
    rounded = expo.astype(jnp.bfloat16).astype(jnp.float32)
    class_num = jnp.einsum("hrl,rlhd->hrd", rounded, value_heads)
    cached_top = jnp.max(class_top, axis=1)
    weight = jnp.exp(class_top - cached_top[:, None])
    cached_total = jnp.sum(weight * class_total, axis=1)
    cached_num = jnp.sum(weight[:, :, None] * class_num, axis=1)
    own_score = jnp.sum(query_heads * key_now.reshape(ATTENTION_HEADS, HEAD_DIM).astype(jnp.float32), axis=1) * score_scale
    highest = jnp.maximum(cached_top, own_score)
    keep = jnp.exp(cached_top - highest)
    own_expo = jnp.exp(own_score - highest)
    totals = cached_total * keep + own_expo
    own_rounded = lax.optimization_barrier(own_expo.astype(jnp.bfloat16)).astype(jnp.float32)
    numerator = cached_num * keep[:, None] + own_rounded[:, None] * value_now.reshape(ATTENTION_HEADS, HEAD_DIM).astype(jnp.float32)
    return (numerator / totals[:, None]).astype(jnp.bfloat16).reshape(ATTENTION_HEADS * HEAD_DIM)


def reference(tokens, key_weight, value_weight, cum_gate, new_input, new_query, new_gate, out_weight):
    batch_rows, length, width = tokens.shape
    flat_rows = tokens.reshape(batch_rows * length, width)
    keys = jnp.dot(flat_rows, key_weight, preferred_element_type=jnp.float32).astype(jnp.bfloat16).reshape(batch_rows, length, width)
    values = jnp.dot(flat_rows, value_weight, preferred_element_type=jnp.float32).astype(jnp.bfloat16).reshape(batch_rows, length, width)
    key_cache = cyclic(keys)
    value_cache = cyclic(values)
    gate_cache = cyclic(cum_gate)
    key_now = jnp.dot(new_input, key_weight, preferred_element_type=jnp.float32).astype(jnp.bfloat16)
    value_now = jnp.dot(new_input, value_weight, preferred_element_type=jnp.float32).astype(jnp.bfloat16)
    attended = lax.map(read_one, (key_cache, value_cache, gate_cache, new_query, new_gate, key_now, value_now))
    grouped = attended.reshape(BATCH_SEQUENCES, N_TP, D // N_TP).astype(jnp.float32)
    weight_groups = out_weight.reshape(N_TP, D // N_TP, D).astype(jnp.float32)
    partial_value = jnp.einsum("bgk,gkn->gbn", grouped, weight_groups)
    partial_value = lax.optimization_barrier(partial_value.astype(jnp.bfloat16)).astype(jnp.float32)
    mixed = jnp.sum(partial_value, axis=0).astype(jnp.bfloat16)
    return (key_cache, value_cache, gate_cache, mixed)
```

```python
import jax
import jax.numpy as jnp
from jax import lax
from jax.experimental import pallas as pl
from jax.experimental.pallas import tpu as pltpu
from jax.sharding import Mesh
from jax.sharding import PartitionSpec as P

MESH = pl.DeviceIdType.MESH
F32 = jnp.float32
BF16 = jnp.bfloat16
NZ, NY, NX, NC = 16, 4, 4, 2
HIGH = lax.Precision.HIGHEST

ORDER = (1, 2, 3, 4, 8, 7, 6, 5)


def slots_of(d):
    if d == 0:
        return 0, 1
    if d == NZ // 2:
        return NZ - 1, 1
    return 2 * d - 1, 2


def iota(shape, dim):
    return lax.broadcasted_iota(jnp.int32, shape, dim)


def nt_dot(a, b, precision=None):
    return lax.dot_general(
        a, b, (((1,), (1,)), ((), ())), precision=precision, preferred_element_type=F32
    )


def fold_heads(wide):
    half = wide[:, :128] + wide[:, 128:]
    return half + pltpu.roll(half, 64, 1)


def merge(parts):
    tops = [p[:, 65:66] for p in parts]
    top = tops[0]
    for t in tops[1:]:
        top = jnp.maximum(top, t)
    total = None
    for p, t in zip(parts, tops):
        term = p * jnp.exp(t - top)
        total = term if total is None else total + term
    lane = iota(total.shape, 1)
    return jnp.where(lane == 65, top, total)


def kernel(
    tok_hbm, wk_hbm, wv_hbm, gate_ref, new_in_ref, query_ref, new_gate_ref, ow_ref,
    k_out, v_out, g_out, m_out,
    tok, wk, wv, part, sent, zbuf, tbuf, g8, pg, zg, yg, ap, ay, azs, az, afs, af, tps, tpr, kv_loc,
    sem_in, d_sem, zs_sem, ys_sem, xs_sem, cs_sem, zr_sem, yr_sem, xr_sem, cr_sem,
    gzs_sem, gzr_sem, gys_sem, gyr_sem, a_send, a_recv,
):
    z, y = lax.axis_index("z"), lax.axis_index("y")
    x, c = lax.axis_index("x"), lax.axis_index("c")
    me = x * NC + c

    def zat(d):
        return lax.rem(z + (d + NZ), NZ)

    def yat(d):
        return lax.rem(y + d, NY)

    def xat(d):
        return lax.rem(x + d, NX)

    def remote(src, dst, ssem, rsem, **dev):
        return pltpu.make_async_remote_copy(
            src_ref=src, dst_ref=dst, send_sem=ssem, recv_sem=rsem,
            device_id=dev, device_id_type=MESH,
        )

    def wait_bytes(ref, sem):
        pltpu.make_async_copy(ref, ref, sem).wait()

    def signal(sem, **dev):
        pl.semaphore_signal(sem, inc=1, device_id=dev, device_id_type=MESH)

    barrier = pltpu.get_barrier_semaphore()
    cols = pl.ds(pl.multiple_of(me * 256, 256), 256)
    load_part = pltpu.make_async_copy(tok_hbm.at[:, :, cols], part, sem_in.at[0])
    load_tok = pltpu.make_async_copy(tok_hbm, tok, sem_in.at[1])
    load_wk = pltpu.make_async_copy(wk_hbm, wk, sem_in.at[2])
    load_wv = pltpu.make_async_copy(wv_hbm, wv, sem_in.at[3])
    load_part.start()
    for dy in range(1, NY):
        signal(barrier, y=yat(dy))
    for dx in range(NX):
        for dc in range(NC):
            if dx or dc:
                signal(barrier, x=xat(dx), c=lax.rem(c + dc, NC))
    for dz in (1, -1):
        signal(barrier, z=zat(dz))
    load_wk.start()
    load_tok.start()
    load_wv.start()

    o, i = iota((512, 512), 0), iota((512, 512), 1)
    perm = (i == ((o & 4) << 6) + ((o & 3) << 6) + (o >> 3)).astype(F32).astype(BF16)
    load_part.wait()
    moved = jnp.dot(perm, part[...].reshape(512, 256), preferred_element_type=F32)
    sent[...] = moved.reshape(NZ, NY, 8, 256).astype(BF16)

    g8[0:4, :] = gate_ref[0]
    g8[4:8, :] = gate_ref[1]
    gates = g8[...]
    lanes, rows = iota((128, 256), 1), iota((128, 256), 0)
    spread = jnp.concatenate(
        [jnp.broadcast_to(gates[k : k + 1, :], (16, 256)) for k in range(8)], axis=0
    )
    same = ((lanes & 3) == ((rows >> 2) & 3)) & ((lanes >> 6) == (rows & 3))
    spread = jnp.where(same, spread, 0.0)
    pick = ((iota((16, 256), 1) >> 2) & 15) == iota((16, 256), 0)
    gate_rows = nt_dot(pick.astype(F32), spread, HIGH)
    for k in range(NZ):
        pg[k] = gate_rows[k : k + 1, :]

    def send_z(d):
        for sign in (1, -1) if d < NZ // 2 else (1,):
            first, count = slots_of(d)
            slot = first if sign < 0 or count == 1 else first + 1
            remote(
                sent.at[zat(sign * d)], zbuf.at[slot], zs_sem, zr_sem.at[d], z=zat(sign * d)
            ).start()
            remote(pg.at[zat(sign * d)], zg.at[z], gzs_sem, gzr_sem, z=zat(sign * d)).start()

    def slots(d):
        first, count = slots_of(d)
        return pl.ds(first, count)

    def y_forward(d):
        if d:
            wait_bytes(zbuf.at[slots(d)], zr_sem.at[d])
        for dy in range(1, NY):
            remote(
                zbuf.at[slots(d), yat(dy)], tbuf.at[me, slots(d), y], ys_sem, yr_sem.at[d],
                y=yat(dy),
            ).start()
        tbuf[me, slots(d), y] = zbuf[slots(d), y]

    def x_forward(d):
        wait_bytes(zbuf.at[slots(d), pl.ds(0, 3)], yr_sem.at[d])
        here = tbuf.at[me, slots(d)]
        for dx in range(1, NX):
            remote(here, here, xs_sem, xr_sem.at[d], x=xat(dx)).start()
        remote(here, here, cs_sem, cr_sem.at[d], c=1 - c).start()

    def c_forward(d):
        wait_bytes(tbuf.at[pl.ds(0, 3), slots(d)], xr_sem.at[d])
        for dx in range(1, NX):
            there = tbuf.at[xat(dx) * NC + c, slots(d)]
            remote(there, there, cs_sem, cr_sem.at[d], c=1 - c).start()

    def finish(ds):
        for d in ds:
            wait_bytes(tbuf.at[pl.ds(0, 4), slots(d)], cr_sem.at[d])
        first = min(slots_of(d)[0] for d in ds)
        count = sum(slots_of(d)[1] for d in ds)
        for w, out in ((wk, k_out), (wv, v_out)):
            acc = None
            for f in range(8):
                lhs = tbuf[f, first : first + count].reshape(count * NY, 8, 256)
                lhs = lhs.astype(F32).reshape(count * 32, 256).astype(BF16)
                term = jnp.dot(
                    lhs, w[f * 256 : (f + 1) * 256, :], preferred_element_type=F32
                )
                acc = term if acc is None else acc + term
            acc = acc.reshape(count * 2, 2, 8, 256)
            even, odd = acc[:, 0], acc[:, 1]
            low = iota(even.shape, 1) < 4
            for b, (a0, a1) in enumerate(
                ((even, pltpu.roll(odd, 4, 1)), (pltpu.roll(even, 4, 1), odd))
            ):
                block = jnp.where(low, a0, a1).reshape(count, 16, 256).astype(BF16)
                for k in range(count):
                    slot = first + k
                    rel = 0 if slot == 0 else 8 if slot == NZ - 1 else (
                        (slot + 1) // 2 if slot % 2 else -(slot // 2)
                    )
                    at = pl.multiple_of(zat(rel) * 16, 16)
                    out[b, pl.ds(at, 16), :] = block[k]

    pl.semaphore_wait(barrier, 3 + 7 + 2)
    for s in (1, -1):
        signal(d_sem.at[0], z=zat(s))
    send_z(1)
    zbuf[0] = sent[z]
    zg[z] = pg[z]
    y_forward(0)
    pl.semaphore_wait(d_sem.at[0], 2)
    for s in (2, -2):
        signal(d_sem.at[1], z=zat(s))
    send_z(2)

    head_of_row = iota((8, 256), 0) & 3
    mine = (iota((8, 256), 1) >> 6) == head_of_row
    second = iota((8, 256), 0) >= 4

    def by_row(two):
        return jnp.where(
            second, jnp.broadcast_to(two[1:2, :], (8, 256)), jnp.broadcast_to(two[0:1, :], (8, 256))
        )

    query = jnp.where(mine, by_row(query_ref[...].astype(F32)), 0.0)
    query_b = query.astype(BF16)
    load_wk.wait()
    load_tok.wait()
    new_in = new_in_ref[...]
    key_now = jnp.dot(new_in, wk[...], preferred_element_type=F32).astype(BF16).astype(F32)
    local = tok[...].reshape(512, 2048)
    kv_loc[...] = jnp.dot(local, wk[...], preferred_element_type=F32).astype(BF16)
    pl.semaphore_wait(d_sem.at[1], 2)
    for s in (4, -4):
        signal(d_sem.at[2], z=zat(s))
    send_z(3)
    send_z(4)
    y_forward(1)
    raw = jnp.where(
        second, nt_dot(query_b, kv_loc[256:, :]), nt_dot(query_b, kv_loc[:256, :])
    )
    ng = new_gate_ref[...]
    ng = jnp.where(
        iota((8, 4), 0) >= 4,
        jnp.broadcast_to(ng[1:2, :], (8, 4)),
        jnp.broadcast_to(ng[0:1, :], (8, 4)),
    )
    ng = jnp.sum(
        jnp.where((iota((8, 4), 0) & 3) == iota((8, 4), 1), ng, 0.0), axis=1, keepdims=True
    )
    scores = raw * 0.125 + ng - g8[...]
    top = jnp.max(scores, axis=1, keepdims=True)
    expo = jnp.exp(scores - top)
    total = jnp.sum(expo, axis=1, keepdims=True)
    expo_b = expo.astype(BF16)
    load_wv.wait()
    value_now = jnp.dot(new_in, wv[...], preferred_element_type=F32).astype(BF16).astype(F32)
    kv_loc[...] = jnp.dot(local, wv[...], preferred_element_type=F32).astype(BF16)
    x_forward(0)
    num = jnp.where(
        second,
        jnp.dot(expo_b, kv_loc[256:, :], preferred_element_type=F32),
        jnp.dot(expo_b, kv_loc[:256, :], preferred_element_type=F32),
    )
    num = fold_heads(jnp.where(mine, num, 0.0))
    lane = iota((8, 128), 1)
    packed = jnp.where(
        lane < 64, num, jnp.where(lane == 64, total, jnp.where(lane == 65, top, 0.0))
    )
    for k in range(NY):
        ap[k] = packed[2 * k : 2 * k + 2, :]
    for dy in range(1, NY):
        remote(ap.at[yat(dy)], ay.at[y], a_send.at[0], a_recv.at[0], y=yat(dy)).start()
    ay[y] = ap[y]
    y_forward(2)
    pl.semaphore_wait(d_sem.at[2], 2)
    send_z(8)
    send_z(7)
    x_forward(1)
    wait_bytes(ay.at[pl.ds(0, 3)], a_recv.at[0])
    merged = merge([ay[k] for k in range(NY)])
    azs[...] = merged
    az[z] = merged
    for d in range(1, NZ):
        remote(azs, az.at[z], a_send.at[1], a_recv.at[1], z=zat(d)).start()
    send_z(6)
    send_z(5)

    y_forward(3)
    c_forward(0)
    x_forward(2)
    y_forward(4)
    c_forward(1)
    x_forward(3)
    c_forward(2)
    x_forward(4)
    c_forward(3)
    c_forward(4)
    finish((0, 1, 2, 3, 4))
    y_forward(8)
    y_forward(7)
    x_forward(8)
    wait_bytes(az.at[pl.ds(0, 15)], a_recv.at[1])
    merged = merge([az[k] for k in range(NZ)])
    afs[...] = merged
    af[y] = merged
    for dy in range(1, NY):
        remote(afs, af.at[y], a_send.at[2], a_recv.at[2], y=yat(dy)).start()
    y_forward(6)
    x_forward(7)
    y_forward(5)
    wait_bytes(zg.at[pl.ds(0, 15)], gzr_sem)
    for dy in range(1, NY):
        remote(zg, yg.at[y], gys_sem, gyr_sem, y=yat(dy)).start()
    for k in range(NZ):
        yg[y, k] = zg[k]
    c_forward(8)
    x_forward(6)
    wait_bytes(af.at[pl.ds(0, 3)], a_recv.at[2])
    cached = jnp.concatenate([af[k] for k in range(NY)], axis=0)
    own = jnp.sum(query * by_row(key_now), axis=1, keepdims=True) * 0.125
    cached_top, cached_total = cached[:, 65:66], cached[:, 64:65]
    cached_num = jnp.where(lane < 64, cached, pltpu.roll(cached, 64, 1))
    highest = jnp.maximum(cached_top, own)
    keep = jnp.exp(cached_top - highest)
    own_expo = jnp.exp(own - highest)
    totals = cached_total * keep + own_expo
    value_rows = fold_heads(jnp.where(mine, by_row(value_now), 0.0))
    numer = cached_num * keep + own_expo.astype(BF16).astype(F32) * value_rows
    attended = (numer / totals).astype(BF16).astype(F32)
    attended = jnp.where(mine, jnp.concatenate([attended, attended], axis=1), 0.0).astype(BF16)
    piece = nt_dot(attended, ow_ref[...])
    piece = jnp.concatenate(
        [jnp.sum(piece[0:4], axis=0, keepdims=True), jnp.sum(piece[4:8], axis=0, keepdims=True)],
        axis=0,
    )
    piece = piece.astype(BF16).astype(F32)
    tps[...] = jnp.concatenate([piece] * 4, axis=1)
    tpr[me] = tps[...]
    for dx in range(NX):
        for dc in range(NC):
            if dx or dc:
                remote(
                    tps, tpr.at[me], a_send.at[3], a_recv.at[3],
                    x=xat(dx), c=lax.rem(c + dc, NC),
                ).start()
    x_forward(5)
    c_forward(7)
    c_forward(6)
    wait_bytes(yg.at[pl.ds(0, 3)], gyr_sem)
    field = (iota((16, 128), 1) >> 2) & 3
    gathered = jnp.zeros((16, 128), F32)
    for k in range(NY):
        rows16 = jnp.concatenate([yg[k, i] for i in range(NZ)], axis=0)
        shift = lax.rem(4 * (k - y) + 128, 128)
        gathered += pltpu.roll(jnp.where(field == y, rows16, 0.0), shift, 1)
    spread = jnp.concatenate(
        [jnp.broadcast_to(gathered[k : k + 1, :], (16, 128)) for k in range(NZ)], axis=0
    )
    same = (iota((256, 128), 0) & 15) == (iota((256, 128), 1) & 15)
    spread = jnp.where(same, spread, 0.0)
    pick = (iota((8, 128), 1) >> 4) == iota((8, 128), 0)
    gate_cols = nt_dot(pick.astype(F32), spread, HIGH)
    g_out[0] = gate_cols[0:4]
    g_out[1] = gate_cols[4:8]
    wait_bytes(tpr.at[pl.ds(0, 7)], a_recv.at[3])
    mixed = tpr[0]
    for k in range(1, NX * NC):
        mixed += tpr[k]
    m_out[...] = mixed[:, :32].astype(BF16)
    c_forward(5)
    finish((5, 6, 7, 8))
    wait_bytes(zbuf.at[pl.ds(0, 15)], zs_sem)
    wait_bytes(zbuf.at[pl.ds(0, 12)], ys_sem)
    wait_bytes(tbuf.at[pl.ds(0, 3)], xs_sem)
    wait_bytes(tbuf.at[pl.ds(0, 4)], cs_sem)
    wait_bytes(zg.at[pl.ds(0, 15)], gzs_sem)
    wait_bytes(yg.at[pl.ds(0, 3)], gys_sem)
    wait_bytes(ap.at[pl.ds(0, 3)], a_send.at[0])
    wait_bytes(az.at[pl.ds(0, 15)], a_send.at[1])
    wait_bytes(af.at[pl.ds(0, 3)], a_send.at[2])
    wait_bytes(tpr.at[pl.ds(0, 7)], a_send.at[3])


def body(tokens, key_weight, value_weight, cum_gate, new_input, new_query, new_gate, out_weight):
    vmem = pl.BlockSpec(memory_space=pltpu.VMEM)
    hbm = pl.BlockSpec(memory_space=pl.ANY)
    dma, regular = pltpu.SemaphoreType.DMA, pltpu.SemaphoreType.REGULAR
    keys, values, gates, mixed = pl.pallas_call(
        kernel,
        out_shape=(
            jax.ShapeDtypeStruct((2, 256, 256), BF16),
            jax.ShapeDtypeStruct((2, 256, 256), BF16),
            jax.ShapeDtypeStruct((2, 4, 256), F32),
            jax.ShapeDtypeStruct((2, 32), BF16),
        ),
        in_specs=[hbm, hbm, hbm, vmem, vmem, vmem, vmem, vmem],
        out_specs=(vmem, vmem, vmem, vmem),
        scratch_shapes=[
            pltpu.VMEM((2, 256, 2048), BF16),
            pltpu.VMEM((2048, 256), BF16),
            pltpu.VMEM((2048, 256), BF16),
            pltpu.VMEM((2, 256, 256), BF16),
            pltpu.VMEM((NZ, NY, 8, 256), BF16),
            pltpu.VMEM((NZ, NY, 8, 256), BF16),
            pltpu.VMEM((8, NZ, NY, 8, 256), BF16),
            pltpu.VMEM((8, 256), F32),
            pltpu.VMEM((NZ, 1, 128), F32),
            pltpu.VMEM((NZ, 1, 128), F32),
            pltpu.VMEM((NY, NZ, 1, 128), F32),
            pltpu.VMEM((NY, 2, 128), F32),
            pltpu.VMEM((NY, 2, 128), F32),
            pltpu.VMEM((2, 128), F32),
            pltpu.VMEM((NZ, 2, 128), F32),
            pltpu.VMEM((2, 128), F32),
            pltpu.VMEM((NY, 2, 128), F32),
            pltpu.VMEM((2, 128), F32),
            pltpu.VMEM((8, 2, 128), F32),
            pltpu.VMEM((512, 256), BF16),
            dma((4,)),
            regular((3,)),
            dma, dma, dma, dma,
            dma((9,)), dma((9,)), dma((9,)), dma((9,)),
            dma, dma, dma, dma,
            dma((4,)), dma((4,)),
        ],
        compiler_params=pltpu.CompilerParams(collective_id=0, has_side_effects=True),
    )(
        tokens, key_weight, value_weight, jnp.swapaxes(cum_gate, 1, 2), new_input, new_query,
        new_gate, out_weight.T,
    )
    return (
        keys.reshape(2, 1, 256, 256),
        values.reshape(2, 1, 256, 256),
        jnp.swapaxes(gates, 1, 2).reshape(2, 1, 256, 4),
        mixed,
    )


def solution(mesh):
    torus = Mesh(mesh.devices.reshape(NZ, NY, NX, NC), ("z", "y", "x", "c"))
    sp, tp = ("z", "y"), ("x", "c")
    return jax.shard_map(
        body,
        mesh=torus,
        in_specs=(
            P(None, sp, None), P(None, tp), P(None, tp), P(None, sp, tp), P(), P(None, tp),
            P(None, tp), P(tp, sp),
        ),
        out_specs=(P(None, sp, None, tp), P(None, sp, None, tp), P(None, sp, None, tp), P(None, sp)),
        check_vma=False,
    )
```

```python
import jax
import jax.numpy as jnp
from jax import lax
from jax.experimental import pallas as pl
from jax.experimental.pallas import tpu as pltpu
from jax.sharding import Mesh
from jax.sharding import PartitionSpec as P

MESH = pl.DeviceIdType.MESH
F32 = jnp.float32
BF16 = jnp.bfloat16
NZ, NY, NX, NC = 16, 4, 4, 2
HIGH = lax.Precision.HIGHEST


def slots_of(d):
    if d == 0:
        return 0, 1
    if d == NZ // 2:
        return NZ - 1, 1
    return 2 * d - 1, 2


def iota(shape, dim):
    return lax.broadcasted_iota(jnp.int32, shape, dim)


def nt_dot(a, b, precision=None):
    return lax.dot_general(
        a, b, (((1,), (1,)), ((), ())), precision=precision, preferred_element_type=F32
    )


def fold_heads(wide):
    half = wide[:, :128] + wide[:, 128:]
    return half + pltpu.roll(half, 64, 1)


def merge(parts):
    tops = [p[:, 65:66] for p in parts]
    top = tops[0]
    for t in tops[1:]:
        top = jnp.maximum(top, t)
    total = None
    for p, t in zip(parts, tops):
        term = p * jnp.exp(t - top)
        total = term if total is None else total + term
    lane = iota(total.shape, 1)
    return jnp.where(lane == 65, top, total)


def kernel(
    tok_hbm, wk_hbm, wv_hbm, gate_hbm, new_in_hbm, query_hbm, new_gate_hbm, ow_hbm,
    k_out, v_out, g_out, m_out,
    tok, wk, wv, part, gate_ref, new_in_ref, query_ref, new_gate_ref, ow_ref,
    order, sent, tbuf, g8, pg, zg, yg, ap, ay, azs, az, afs, af, tps, tpr, kv_loc,
    sem_in, d_sem, zs_sem, ys_sem, xs_sem, cs_sem, zr_sem, xl_sem, xh_sem, x2_sem, cr_sem,
    gzs_sem, gzr_sem, gys_sem, gyr_sem, a_send, a_recv,
):
    z, y = lax.axis_index("z"), lax.axis_index("y")
    x, c = lax.axis_index("x"), lax.axis_index("c")
    me = x * NC + c

    def zat(d):
        return lax.rem(z + (d + NZ), NZ)

    def yat(d):
        return lax.rem(y + d, NY)

    def xat(d):
        return lax.rem(x + (d + NX), NX)

    def remote(src, dst, ssem, rsem, **dev):
        return pltpu.make_async_remote_copy(
            src_ref=src, dst_ref=dst, send_sem=ssem, recv_sem=rsem,
            device_id=dev, device_id_type=MESH,
        )

    def wait_bytes(ref, sem):
        pltpu.make_async_copy(ref, ref, sem).wait()

    def signal(sem, **dev):
        pl.semaphore_signal(sem, inc=1, device_id=dev, device_id_type=MESH)

    barrier = pltpu.get_barrier_semaphore()
    cols = pl.ds(pl.multiple_of(me * 256, 256), 256)
    sources = (
        (tok_hbm.at[:, :, cols], part), (tok_hbm, tok), (wk_hbm, wk), (wv_hbm, wv),
        (gate_hbm, gate_ref), (new_in_hbm, new_in_ref), (query_hbm, query_ref),
        (new_gate_hbm, new_gate_ref), (ow_hbm, ow_ref),
    )
    loads = [pltpu.make_async_copy(s, d, sem_in.at[k]) for k, (s, d) in enumerate(sources)]
    load_part, load_tok, load_wk, load_wv, load_gate, load_in, load_q, load_ng, load_ow = loads
    load_part.start()
    for dz in (1, -1):
        for dy in range(NY):
            signal(barrier, z=zat(dz), y=yat(dy))
    for dy in range(1, NY):
        signal(barrier, y=yat(dy))
    for dx in range(NX):
        for dc in range(NC):
            if dx or dc:
                signal(barrier, x=xat(dx), c=lax.rem(c + dc, NC))
    for load in (load_gate, load_q, load_ng, load_in, load_wk, load_tok, load_wv, load_ow):
        load.start()

    def send_z(d):
        for sign in (1, -1) if d < NZ // 2 else (1,):
            first, count = slots_of(d)
            slot = first if sign < 0 or count == 1 else first + 1
            to = zat(sign * d)
            for dy in range(NY):
                remote(
                    sent.at[to, yat(dy)], tbuf.at[me, slot, y], zs_sem, zr_sem.at[d],
                    z=to, y=yat(dy),
                ).start()

    def slots(d):
        first, count = slots_of(d)
        return pl.ds(first, count)

    def half(f, d, upper):
        first, count = slots_of(d)
        if count == 2:
            return tbuf.at[f, pl.ds(first + upper, 1)]
        return tbuf.at[f, pl.ds(first, 1), pl.ds(2 * upper, 2)]

    low_f, high_f = xat(-1) * NC + c, xat(1) * NC + c

    def x_first(d):
        here = tbuf.at[me, slots(d)]
        if d:
            wait_bytes(here, zr_sem.at[d])
        else:
            wait_bytes(tbuf.at[me, 0, pl.ds(0, 3)], zr_sem.at[0])
        remote(here, here, xs_sem, xl_sem.at[d], x=xat(1)).start()
        remote(here, here, xs_sem, xh_sem.at[d], x=xat(-1)).start()
        remote(here, here, cs_sem, cr_sem.at[d], c=1 - c).start()

    def x_second(d):
        for f, sem, upper, to in ((low_f, xl_sem, 0, xat(1)), (high_f, xh_sem, 1, xat(-1))):
            came = tbuf.at[f, slots(d)]
            wait_bytes(came, sem.at[d])
            piece = half(f, d, upper)
            for core in range(NC):
                remote(piece, piece, xs_sem, x2_sem.at[d], x=to, c=lax.rem(c + core, NC)).start()
            remote(came, came, cs_sem, cr_sem.at[d], c=1 - c).start()

    def finish(ds):
        for d in ds:
            wait_bytes(tbuf.at[pl.ds(0, 3), slots(d)], cr_sem.at[d])
            wait_bytes(tbuf.at[pl.ds(0, 2), slots(d)], x2_sem.at[d])
        first = min(slots_of(d)[0] for d in ds)
        count = sum(slots_of(d)[1] for d in ds)
        for w, out in ((wk, k_out), (wv, v_out)):
            acc = None
            for f in range(8):
                lhs = tbuf[f, first : first + count].reshape(count * NY, 8, 256)
                lhs = lhs.astype(F32).reshape(count * 32, 256).astype(BF16)
                term = jnp.dot(
                    lhs, w[f * 256 : (f + 1) * 256, :], preferred_element_type=F32
                )
                acc = term if acc is None else acc + term
            acc = acc.reshape(count * 2, 2, 8, 256)
            even, odd = acc[:, 0], acc[:, 1]
            low = iota(even.shape, 1) < 4
            for b, (a0, a1) in enumerate(
                ((even, pltpu.roll(odd, 4, 1)), (pltpu.roll(even, 4, 1), odd))
            ):
                block = jnp.where(low, a0, a1).reshape(count, 16, 256).astype(BF16)
                for k in range(count):
                    slot = first + k
                    rel = 0 if slot == 0 else 8 if slot == NZ - 1 else (
                        (slot + 1) // 2 if slot % 2 else -(slot // 2)
                    )
                    at = pl.multiple_of(zat(rel) * 16, 16)
                    out[b, pl.ds(at, 16), :] = block[k]

    pl.semaphore_wait(barrier, 3 + 7 + 8)
    for s in (1, -1):
        signal(d_sem.at[0], z=zat(s))
    load_part.wait()
    for b in range(2):
        for j in range(4):
            for k in range(2):
                order[k, pl.ds(4 * b + j, 64, stride=8), :] = part[
                    b, 64 * j : 64 * j + 64, 128 * k : 128 * k + 128
                ].astype(F32)
    for k in range(2):
        sent[:, :, :, 128 * k : 128 * k + 128] = order[k].reshape(NZ, NY, 8, 128).astype(BF16)
    for dy in range(1, NY):
        remote(
            sent.at[z, yat(dy)], tbuf.at[me, 0, y], ys_sem, zr_sem.at[0], y=yat(dy)
        ).start()
    send_z(1)
    tbuf[me, 0, y] = sent[z, y]
    pl.semaphore_wait(d_sem.at[0], 2)
    for s in (2, -2):
        signal(d_sem.at[1], z=zat(s))
    send_z(2)

    load_gate.wait()
    g8[0:4, :] = gate_ref[0]
    g8[4:8, :] = gate_ref[1]
    gates = g8[...]
    lanes, rows = iota((128, 256), 1), iota((128, 256), 0)
    spread = jnp.concatenate(
        [jnp.broadcast_to(gates[k : k + 1, :], (16, 256)) for k in range(8)], axis=0
    )
    same = ((lanes & 3) == ((rows >> 2) & 3)) & ((lanes >> 6) == (rows & 3))
    spread = jnp.where(same, spread, 0.0)
    pick = ((iota((16, 256), 1) >> 2) & 15) == iota((16, 256), 0)
    gate_rows = nt_dot(pick.astype(F32), spread, HIGH)
    for k in range(NZ):
        pg[k] = gate_rows[k : k + 1, :]

    head_of_row = iota((8, 256), 0) & 3
    mine = (iota((8, 256), 1) >> 6) == head_of_row
    second = iota((8, 256), 0) >= 4

    def by_row(two):
        return jnp.where(
            second, jnp.broadcast_to(two[1:2, :], (8, 256)), jnp.broadcast_to(two[0:1, :], (8, 256))
        )

    for load in (load_q, load_ng, load_in):
        load.wait()
    query = jnp.where(mine, by_row(query_ref[...].astype(F32)), 0.0)
    query_b = query.astype(BF16)
    new_in = new_in_ref[...]
    pl.semaphore_wait(d_sem.at[1], 2)
    for s in (4, -4):
        signal(d_sem.at[2], z=zat(s))
    send_z(3)
    send_z(4)
    x_first(0)
    x_first(1)
    load_wk.wait()
    load_tok.wait()
    key_now = jnp.dot(new_in, wk[...], preferred_element_type=F32).astype(BF16).astype(F32)
    local = tok[...].reshape(512, 2048)
    kv_loc[...] = jnp.dot(local, wk[...], preferred_element_type=F32).astype(BF16)
    x_second(0)
    raw = jnp.where(
        second, nt_dot(query_b, kv_loc[256:, :]), nt_dot(query_b, kv_loc[:256, :])
    )
    ng = new_gate_ref[...]
    ng = jnp.where(
        iota((8, 4), 0) >= 4,
        jnp.broadcast_to(ng[1:2, :], (8, 4)),
        jnp.broadcast_to(ng[0:1, :], (8, 4)),
    )
    ng = jnp.sum(
        jnp.where((iota((8, 4), 0) & 3) == iota((8, 4), 1), ng, 0.0), axis=1, keepdims=True
    )
    scores = raw * 0.125 + ng - g8[...]
    top = jnp.max(scores, axis=1, keepdims=True)
    expo = jnp.exp(scores - top)
    total = jnp.sum(expo, axis=1, keepdims=True)
    expo_b = expo.astype(BF16)
    load_wv.wait()
    kv_loc[...] = jnp.dot(local, wv[...], preferred_element_type=F32).astype(BF16)
    x_first(2)
    x_second(1)
    num = jnp.where(
        second,
        jnp.dot(expo_b, kv_loc[256:, :], preferred_element_type=F32),
        jnp.dot(expo_b, kv_loc[:256, :], preferred_element_type=F32),
    )
    num = fold_heads(jnp.where(mine, num, 0.0))
    lane = iota((8, 128), 1)
    packed = jnp.where(
        lane < 64, num, jnp.where(lane == 64, total, jnp.where(lane == 65, top, 0.0))
    )
    for k in range(NY):
        ap[k] = packed[2 * k : 2 * k + 2, :]
    for dy in range(1, NY):
        remote(ap.at[yat(dy)], ay.at[y], a_send.at[0], a_recv.at[0], y=yat(dy)).start()
    ay[y] = ap[y]
    pl.semaphore_wait(d_sem.at[2], 2)
    send_z(8)
    send_z(7)
    zg[z] = pg[z]
    for d in range(1, NZ):
        remote(pg.at[zat(d)], zg.at[z], gzs_sem, gzr_sem, z=zat(d)).start()
    value_now = jnp.dot(new_in, wv[...], preferred_element_type=F32).astype(BF16).astype(F32)
    x_first(3)
    x_second(2)
    wait_bytes(ay.at[pl.ds(0, 3)], a_recv.at[0])
    merged = merge([ay[k] for k in range(NY)])
    azs[...] = merged
    az[z] = merged
    for d in range(1, NZ):
        remote(azs, az.at[z], a_send.at[1], a_recv.at[1], z=zat(d)).start()
    send_z(6)
    send_z(5)
    x_first(4)
    x_second(3)
    finish((0, 1, 2, 3))
    x_second(4)
    x_first(8)
    x_first(7)
    wait_bytes(az.at[pl.ds(0, 15)], a_recv.at[1])
    merged = merge([az[k] for k in range(NZ)])
    afs[...] = merged
    af[y] = merged
    for dy in range(1, NY):
        remote(afs, af.at[y], a_send.at[2], a_recv.at[2], y=yat(dy)).start()
    x_second(8)
    x_first(6)
    wait_bytes(zg.at[pl.ds(0, 15)], gzr_sem)
    for dy in range(1, NY):
        remote(zg, yg.at[y], gys_sem, gyr_sem, y=yat(dy)).start()
    for k in range(NZ):
        yg[y, k] = zg[k]
    x_second(7)
    x_first(5)
    load_ow.wait()
    wait_bytes(af.at[pl.ds(0, 3)], a_recv.at[2])
    cached = jnp.concatenate([af[k] for k in range(NY)], axis=0)
    own = jnp.sum(query * by_row(key_now), axis=1, keepdims=True) * 0.125
    cached_top, cached_total = cached[:, 65:66], cached[:, 64:65]
    cached_num = jnp.where(lane < 64, cached, pltpu.roll(cached, 64, 1))
    highest = jnp.maximum(cached_top, own)
    keep = jnp.exp(cached_top - highest)
    own_expo = jnp.exp(own - highest)
    totals = cached_total * keep + own_expo
    value_rows = fold_heads(jnp.where(mine, by_row(value_now), 0.0))
    numer = cached_num * keep + own_expo.astype(BF16).astype(F32) * value_rows
    attended = (numer / totals).astype(BF16).astype(F32)
    attended = jnp.where(mine, jnp.concatenate([attended, attended], axis=1), 0.0).astype(BF16)
    piece = nt_dot(attended, ow_ref[...])
    piece = jnp.concatenate(
        [jnp.sum(piece[0:4], axis=0, keepdims=True), jnp.sum(piece[4:8], axis=0, keepdims=True)],
        axis=0,
    )
    piece = piece.astype(BF16).astype(F32)
    tps[...] = jnp.concatenate([piece] * 4, axis=1)
    tpr[me] = tps[...]
    for dx in range(NX):
        for dc in range(NC):
            if dx or dc:
                remote(
                    tps, tpr.at[me], a_send.at[3], a_recv.at[3],
                    x=xat(dx), c=lax.rem(c + dc, NC),
                ).start()
    x_second(6)
    x_second(5)
    wait_bytes(yg.at[pl.ds(0, 3)], gyr_sem)
    field = (iota((16, 128), 1) >> 2) & 3
    gathered = jnp.zeros((16, 128), F32)
    for k in range(NY):
        rows16 = jnp.concatenate([yg[k, i] for i in range(NZ)], axis=0)
        shift = lax.rem(4 * (k - y) + 128, 128)
        gathered += pltpu.roll(jnp.where(field == y, rows16, 0.0), shift, 1)
    spread = jnp.concatenate(
        [jnp.broadcast_to(gathered[k : k + 1, :], (16, 128)) for k in range(NZ)], axis=0
    )
    same = (iota((256, 128), 0) & 15) == (iota((256, 128), 1) & 15)
    spread = jnp.where(same, spread, 0.0)
    pick = (iota((8, 128), 1) >> 4) == iota((8, 128), 0)
    gate_cols = nt_dot(pick.astype(F32), spread, HIGH)
    g_out[0] = gate_cols[0:4]
    g_out[1] = gate_cols[4:8]
    wait_bytes(tpr.at[pl.ds(0, 7)], a_recv.at[3])
    mixed = tpr[0]
    for k in range(1, NX * NC):
        mixed += tpr[k]
    m_out[...] = mixed[:, :32].astype(BF16)
    finish((4, 5, 6, 7, 8))
    wait_bytes(tbuf.at[0, pl.ds(0, 15)], zs_sem)
    wait_bytes(tbuf.at[0, 0, pl.ds(0, 3)], ys_sem)
    wait_bytes(tbuf.at[pl.ds(0, 4)], xs_sem)
    wait_bytes(tbuf.at[pl.ds(0, 3)], cs_sem)
    wait_bytes(zg.at[pl.ds(0, 15)], gzs_sem)
    wait_bytes(yg.at[pl.ds(0, 3)], gys_sem)
    wait_bytes(ap.at[pl.ds(0, 3)], a_send.at[0])
    wait_bytes(az.at[pl.ds(0, 15)], a_send.at[1])
    wait_bytes(af.at[pl.ds(0, 3)], a_send.at[2])
    wait_bytes(tpr.at[pl.ds(0, 7)], a_send.at[3])


def put_out(*refs):
    ins, outs, sem = refs[:4], refs[4:8], refs[8]
    copies = [
        pltpu.make_async_copy(i, o, sem.at[k]) for k, (i, o) in enumerate(zip(ins, outs))
    ]
    for copy in copies:
        copy.start()
    for copy in copies:
        copy.wait()


def body(tokens, key_weight, value_weight, cum_gate, new_input, new_query, new_gate, out_weight):
    vmem = pl.BlockSpec(memory_space=pltpu.VMEM)
    hbm = pl.BlockSpec(memory_space=pltpu.HBM)
    dma, regular = pltpu.SemaphoreType.DMA, pltpu.SemaphoreType.REGULAR
    shapes = (
        jax.ShapeDtypeStruct((2, 256, 256), BF16),
        jax.ShapeDtypeStruct((2, 256, 256), BF16),
        jax.ShapeDtypeStruct((2, 4, 256), F32),
        jax.ShapeDtypeStruct((2, 32), BF16),
    )
    results = pl.pallas_call(
        kernel,
        out_shape=shapes,
        in_specs=[hbm] * 8,
        out_specs=(vmem,) * 4,
        scratch_shapes=[
            pltpu.VMEM((2, 256, 2048), BF16),
            pltpu.VMEM((2048, 256), BF16),
            pltpu.VMEM((2048, 256), BF16),
            pltpu.VMEM((2, 256, 256), BF16),
            pltpu.VMEM((2, 4, 256), F32),
            pltpu.VMEM((2, 2048), BF16),
            pltpu.VMEM((2, 256), BF16),
            pltpu.VMEM((2, 4), F32),
            pltpu.VMEM((32, 256), BF16),
            pltpu.VMEM((2, 512, 128), F32),
            pltpu.VMEM((NZ, NY, 8, 256), BF16),
            pltpu.VMEM((8, NZ, NY, 8, 256), BF16),
            pltpu.VMEM((8, 256), F32),
            pltpu.VMEM((NZ, 1, 128), F32),
            pltpu.VMEM((NZ, 1, 128), F32),
            pltpu.VMEM((NY, NZ, 1, 128), F32),
            pltpu.VMEM((NY, 2, 128), F32),
            pltpu.VMEM((NY, 2, 128), F32),
            pltpu.VMEM((2, 128), F32),
            pltpu.VMEM((NZ, 2, 128), F32),
            pltpu.VMEM((2, 128), F32),
            pltpu.VMEM((NY, 2, 128), F32),
            pltpu.VMEM((2, 128), F32),
            pltpu.VMEM((8, 2, 128), F32),
            pltpu.VMEM((512, 256), BF16),
            dma((9,)),
            regular((3,)),
            dma, dma, dma, dma,
            dma((9,)), dma((9,)), dma((9,)), dma((9,)), dma((9,)),
            dma, dma, dma, dma,
            dma((4,)), dma((4,)),
        ],
        compiler_params=pltpu.CompilerParams(
            collective_id=0, has_side_effects=True, vmem_limit_bytes=24 * 2**20
        ),
    )(
        *(
            pltpu.with_memory_space_constraint(a, pltpu.HBM)
            for a in (
                tokens, key_weight, value_weight, jnp.swapaxes(cum_gate, 1, 2), new_input,
                new_query, new_gate, out_weight.T,
            )
        )
    )
    keys, values, gates, mixed = pl.pallas_call(
        put_out,
        out_shape=shapes,
        in_specs=[vmem] * 4,
        out_specs=(hbm,) * 4,
        scratch_shapes=[dma((4,))],
        compiler_params=pltpu.CompilerParams(vmem_limit_bytes=4 * 2**20),
    )(*results)
    return (
        keys.reshape(2, 1, 256, 256),
        values.reshape(2, 1, 256, 256),
        jnp.swapaxes(gates, 1, 2).reshape(2, 1, 256, 4),
        mixed,
    )


def solution(mesh):
    torus = Mesh(mesh.devices.reshape(NZ, NY, NX, NC), ("z", "y", "x", "c"))
    sp, tp = ("z", "y"), ("x", "c")
    return jax.shard_map(
        body,
        mesh=torus,
        in_specs=(
            P(None, sp, None), P(None, tp), P(None, tp), P(None, sp, tp), P(), P(None, tp),
            P(None, tp), P(tp, sp),
        ),
        out_specs=(P(None, sp, None, tp), P(None, sp, None, tp), P(None, sp, None, tp), P(None, sp)),
        check_vma=False,
    )
```

```python
import jax
import jax.numpy as jnp
from jax import lax
from jax.experimental import pallas as pl
from jax.experimental.pallas import tpu as pltpu
from jax.sharding import Mesh
from jax.sharding import PartitionSpec as P

MESH = pl.DeviceIdType.MESH
F32 = jnp.float32
BF16 = jnp.bfloat16
NZ, NY, NX, NC = 16, 4, 4, 2
HIGH = lax.Precision.HIGHEST
FAR = 4


def slots_of(d):
    if d == 0:
        return 0, 1
    if d == NZ // 2:
        return NZ - 1, 1
    return 2 * d - 1, 2


def iota(shape, dim):
    return lax.broadcasted_iota(jnp.int32, shape, dim)


def nt_dot(a, b, precision=None):
    return lax.dot_general(
        a, b, (((1,), (1,)), ((), ())), precision=precision, preferred_element_type=F32
    )


def fold_heads(wide):
    half = wide[:, :128] + wide[:, 128:]
    return half + pltpu.roll(half, 64, 1)


def merge(parts):
    tops = [p[:, 65:66] for p in parts]
    top = tops[0]
    for t in tops[1:]:
        top = jnp.maximum(top, t)
    total = None
    for p, t in zip(parts, tops):
        term = p * jnp.exp(t - top)
        total = term if total is None else total + term
    lane = iota(total.shape, 1)
    return jnp.where(lane == 65, top, total)


def kernel(
    tok_hbm, wk_hbm, wv_hbm, gate_hbm, new_in_hbm, query_hbm, new_gate_hbm, ow_hbm,
    k_out, v_out, g_out, m_out,
    tok, wk, wv, part, gate_ref, new_in_ref, query_ref, new_gate_ref, ow_ref,
    order, sent, tbuf, relay, g8, pg, zg, yg, grelay, azs, az, far, afs, af, tps, tpr, kv_loc,
    sem_in, d_sem, zs_sem, ys_sem, ls_sem, rs_sem, xs_sem, cs_sem, zr_sem, lr_sem, xr_sem, cr_sem,
    gzs_sem, gzr_sem, grs_sem, grr_sem, gys_sem, gyr_sem, a_send, a_recv,
):
    z, y = lax.axis_index("z"), lax.axis_index("y")
    x, c = lax.axis_index("x"), lax.axis_index("c")
    me = x * NC + c

    def zat(d):
        return lax.rem(z + (d + NZ), NZ)

    def yat(d):
        return lax.rem(y + d, NY)

    def xat(d):
        return lax.rem(x + (d + NX), NX)

    def remote(src, dst, ssem, rsem, **dev):
        return pltpu.make_async_remote_copy(
            src_ref=src, dst_ref=dst, send_sem=ssem, recv_sem=rsem,
            device_id=dev, device_id_type=MESH,
        )

    def wait_bytes(ref, sem):
        pltpu.make_async_copy(ref, ref, sem).wait()

    def signal(sem, **dev):
        pl.semaphore_signal(sem, inc=1, device_id=dev, device_id_type=MESH)

    barrier = pltpu.get_barrier_semaphore()
    cols = pl.ds(pl.multiple_of(me * 256, 256), 256)
    sources = (
        (tok_hbm.at[:, :, cols], part), (tok_hbm, tok), (wk_hbm, wk), (wv_hbm, wv),
        (gate_hbm, gate_ref), (new_in_hbm, new_in_ref), (query_hbm, query_ref),
        (new_gate_hbm, new_gate_ref), (ow_hbm, ow_ref),
    )
    loads = [pltpu.make_async_copy(s, d, sem_in.at[k]) for k, (s, d) in enumerate(sources)]
    load_part, load_tok, load_wk, load_wv, load_gate, load_in, load_q, load_ng, load_ow = loads
    load_part.start()
    for dz in (1, -1):
        for dy in range(NY):
            signal(barrier, z=zat(dz), y=yat(dy))
    for dy in range(1, NY):
        signal(barrier, y=yat(dy))
    for dx in range(NX):
        for dc in range(NC):
            if dx or dc:
                signal(barrier, x=xat(dx), c=lax.rem(c + dc, NC))
    for load in (load_gate, load_q, load_ng, load_in, load_wk, load_tok, load_wv, load_ow):
        load.start()

    def slot_at(d, sign):
        first, count = slots_of(d)
        return first + 1 if sign > 0 and count == 2 else first

    def send_z(d):
        for sign in (1, -1):
            to = zat(sign * d)
            for dy in range(NY):
                remote(
                    sent.at[to, yat(dy)], tbuf.at[me, slot_at(d, sign), y], zs_sem, zr_sem.at[d],
                    z=to, y=yat(dy),
                ).start()

    def to_relay(k):
        for way, sign in enumerate((1, -1)):
            to = zat(sign * (FAR + k))
            if k < FAR:
                src, dst = sent.at[to], relay.at[way, k - 1]
            else:
                src, dst = sent.at[to, pl.ds(2 * way, 2)], relay.at[way, k - 1, pl.ds(0, 2)]
            remote(src, dst, ls_sem, lr_sem.at[k], z=zat(sign * FAR)).start()

    def pass_on(k):
        came = relay.at[:, k - 1] if k < FAR else relay.at[:, k - 1, pl.ds(0, 2)]
        wait_bytes(came, lr_sem.at[k])
        for way, sign in enumerate((1, -1)):
            for q in range(NY if k < FAR else 2):
                remote(
                    relay.at[way, k - 1, q], tbuf.at[me, slot_at(FAR + k, sign), y], rs_sem,
                    zr_sem.at[FAR + k], z=zat(sign * k), y=q if k < FAR else q + 2 * way,
                ).start()

    def slots(d):
        first, count = slots_of(d)
        return pl.ds(first, count)

    def x_first(d):
        here = tbuf.at[me, slots(d)]
        if d:
            wait_bytes(here, zr_sem.at[d])
        else:
            wait_bytes(tbuf.at[me, 0, pl.ds(0, 3)], zr_sem.at[0])
        for dx in (1, -1, 2):
            remote(here, here, xs_sem, xr_sem.at[d], x=xat(dx)).start()
        remote(here, here, cs_sem, cr_sem.at[d], c=1 - c).start()

    def x_second(d):
        wait_bytes(tbuf.at[pl.ds(0, 3), slots(d)], xr_sem.at[d])
        for dx in range(1, NX):
            came = tbuf.at[xat(dx) * NC + c, slots(d)]
            remote(came, came, cs_sem, cr_sem.at[d], c=1 - c).start()

    def finish(ds):
        for d in ds:
            wait_bytes(tbuf.at[pl.ds(0, 4), slots(d)], cr_sem.at[d])
        first = min(slots_of(d)[0] for d in ds)
        count = sum(slots_of(d)[1] for d in ds)
        for w, out in ((wk, k_out), (wv, v_out)):
            acc = None
            for f in range(8):
                lhs = tbuf[f, first : first + count].reshape(count * NY, 8, 256)
                lhs = lhs.astype(F32).reshape(count * 32, 256).astype(BF16)
                term = jnp.dot(
                    lhs, w[f * 256 : (f + 1) * 256, :], preferred_element_type=F32
                )
                acc = term if acc is None else acc + term
            acc = acc.reshape(count * 2, 2, 8, 256)
            even, odd = acc[:, 0], acc[:, 1]
            low = iota(even.shape, 1) < 4
            for b, (a0, a1) in enumerate(
                ((even, pltpu.roll(odd, 4, 1)), (pltpu.roll(even, 4, 1), odd))
            ):
                block = jnp.where(low, a0, a1).reshape(count, 16, 256).astype(BF16)
                for k in range(count):
                    slot = first + k
                    rel = 0 if slot == 0 else 8 if slot == NZ - 1 else (
                        (slot + 1) // 2 if slot % 2 else -(slot // 2)
                    )
                    at = pl.multiple_of(zat(rel) * 16, 16)
                    out[b, pl.ds(at, 16), :] = block[k]

    pl.semaphore_wait(barrier, 3 + 7 + 8)
    for s in (1, -1):
        signal(d_sem.at[0], z=zat(s))
    load_part.wait()
    for b in range(2):
        for j in range(4):
            for k in range(2):
                order[k, pl.ds(4 * b + j, 64, stride=8), :] = part[
                    b, 64 * j : 64 * j + 64, 128 * k : 128 * k + 128
                ].astype(F32)
    for k in range(2):
        sent[:, :, :, 128 * k : 128 * k + 128] = order[k].reshape(NZ, NY, 8, 128).astype(BF16)
    for dy in range(1, NY):
        remote(
            sent.at[z, yat(dy)], tbuf.at[me, 0, y], ys_sem, zr_sem.at[0], y=yat(dy)
        ).start()
    send_z(1)
    tbuf[me, 0, y] = sent[z, y]
    pl.semaphore_wait(d_sem.at[0], 2)
    for s in (2, -2):
        signal(d_sem.at[1], z=zat(s))
    send_z(2)

    pl.semaphore_wait(d_sem.at[1], 2)
    to_relay(1)
    to_relay(2)
    head_of_row = iota((8, 256), 0) & 3
    mine = (iota((8, 256), 1) >> 6) == head_of_row
    second = iota((8, 256), 0) >= 4

    def by_row(two):
        return jnp.where(
            second, jnp.broadcast_to(two[1:2, :], (8, 256)), jnp.broadcast_to(two[0:1, :], (8, 256))
        )

    for load in (load_q, load_ng, load_in):
        load.wait()
    query = jnp.where(mine, by_row(query_ref[...].astype(F32)), 0.0)
    query_b = query.astype(BF16)
    new_in = new_in_ref[...]
    load_gate.wait()
    g8[0:4, :] = gate_ref[0]
    g8[4:8, :] = gate_ref[1]
    gates = g8[...]
    lanes, rows = iota((128, 256), 1), iota((128, 256), 0)
    spread = jnp.concatenate(
        [jnp.broadcast_to(gates[k : k + 1, :], (16, 256)) for k in range(8)], axis=0
    )
    same = ((lanes & 3) == ((rows >> 2) & 3)) & ((lanes >> 6) == (rows & 3))
    spread = jnp.where(same, spread, 0.0)
    pick = ((iota((16, 256), 1) >> 2) & 15) == iota((16, 256), 0)
    gate_rows = nt_dot(pick.astype(F32), spread, HIGH)
    for k in range(NZ):
        pg[k] = gate_rows[k : k + 1, :]

    to_relay(4)
    load_wk.wait()
    load_tok.wait()
    key_now = jnp.dot(new_in, wk[...], preferred_element_type=F32).astype(BF16).astype(F32)
    local = tok[...].reshape(512, 2048)
    kv_loc[...] = jnp.dot(local, wk[...], preferred_element_type=F32).astype(BF16)
    raw = jnp.where(
        second, nt_dot(query_b, kv_loc[256:, :]), nt_dot(query_b, kv_loc[:256, :])
    )
    ng = new_gate_ref[...]
    ng = jnp.where(
        iota((8, 4), 0) >= 4,
        jnp.broadcast_to(ng[1:2, :], (8, 4)),
        jnp.broadcast_to(ng[0:1, :], (8, 4)),
    )
    ng = jnp.sum(
        jnp.where((iota((8, 4), 0) & 3) == iota((8, 4), 1), ng, 0.0), axis=1, keepdims=True
    )
    scores = raw * 0.125 + ng - g8[...]
    top = jnp.max(scores, axis=1, keepdims=True)
    expo = jnp.exp(scores - top)
    total = jnp.sum(expo, axis=1, keepdims=True)
    expo_b = expo.astype(BF16)
    x_first(1)
    x_first(0)
    load_wv.wait()
    kv_loc[...] = jnp.dot(local, wv[...], preferred_element_type=F32).astype(BF16)
    x_first(2)
    send_z(3)
    num = jnp.where(
        second,
        jnp.dot(expo_b, kv_loc[256:, :], preferred_element_type=F32),
        jnp.dot(expo_b, kv_loc[:256, :], preferred_element_type=F32),
    )
    num = fold_heads(jnp.where(mine, num, 0.0))
    lane = iota((8, 128), 1)
    packed = jnp.where(
        lane < 64, num, jnp.where(lane == 64, total, jnp.where(lane == 65, top, 0.0))
    )
    azs[...] = packed
    for d in range(1, FAR + 1):
        for sign in (1, -1):
            slot = d - 1 if sign < 0 else FAR + d - 1
            remote(azs, az.at[slot], a_send.at[0], a_recv.at[0], z=zat(sign * d)).start()
    to_relay(3)
    x_second(0)
    x_second(1)
    pass_on(1)
    send_z(4)
    pass_on(2)
    x_first(3)
    zg[z] = pg[z]
    for sign in (1, -1):
        for d in range(1, FAR + 1):
            remote(pg.at[zat(sign * d)], zg.at[z], gzs_sem, gzr_sem, z=zat(sign * d)).start()
    for way, sign in enumerate((1, -1)):
        for k in range(1, FAR + 1 - way):
            remote(
                pg.at[zat(sign * (FAR + k))], grelay.at[FAR * way + k - 1], gzs_sem, grr_sem,
                z=zat(sign * FAR),
            ).start()
    wait_bytes(az.at[pl.ds(0, 8)], a_recv.at[0])
    far[0] = merge([az[k] for k in range(FAR)])
    far[1] = merge([az[k] for k in range(FAR, 2 * FAR - 1)])
    remote(far.at[0], az.at[8], a_send.at[1], a_recv.at[1], z=zat(-FAR)).start()
    remote(far.at[1], az.at[9], a_send.at[1], a_recv.at[1], z=zat(FAR)).start()
    pass_on(3)
    x_first(5)
    pass_on(4)
    x_first(6)
    x_first(4)
    wait_bytes(zg.at[pl.ds(0, 7)], grr_sem)
    for way, sign in enumerate((1, -1)):
        for k in range(1, FAR + 1 - way):
            remote(
                grelay.at[FAR * way + k - 1], zg.at[zat(-sign * FAR)], grs_sem, gzr_sem,
                z=zat(sign * k),
            ).start()
    wait_bytes(az.at[pl.ds(8, 2)], a_recv.at[1])
    merged = merge([azs[...]] + [az[k] for k in range(10)])
    afs[...] = merged
    af[y] = merged
    for dy in range(1, NY):
        remote(afs, af.at[y], a_send.at[2], a_recv.at[2], y=yat(dy)).start()
    x_first(7)
    x_first(8)
    x_second(2)
    x_second(3)
    value_now = jnp.dot(new_in, wv[...], preferred_element_type=F32).astype(BF16).astype(F32)
    x_second(5)
    x_second(6)
    load_ow.wait()
    wait_bytes(af.at[pl.ds(0, 3)], a_recv.at[2])
    cached = merge([af[k] for k in range(NY)])
    own = jnp.sum(query * by_row(key_now), axis=1, keepdims=True) * 0.125
    cached_top, cached_total = cached[:, 65:66], cached[:, 64:65]
    cached_num = jnp.where(lane < 64, cached, pltpu.roll(cached, 64, 1))
    highest = jnp.maximum(cached_top, own)
    keep = jnp.exp(cached_top - highest)
    own_expo = jnp.exp(own - highest)
    totals = cached_total * keep + own_expo
    value_rows = fold_heads(jnp.where(mine, by_row(value_now), 0.0))
    numer = cached_num * keep + own_expo.astype(BF16).astype(F32) * value_rows
    attended = (numer / totals).astype(BF16).astype(F32)
    attended = jnp.where(mine, jnp.concatenate([attended, attended], axis=1), 0.0).astype(BF16)
    piece = nt_dot(attended, ow_ref[...])
    piece = jnp.concatenate(
        [jnp.sum(piece[0:4], axis=0, keepdims=True), jnp.sum(piece[4:8], axis=0, keepdims=True)],
        axis=0,
    )
    piece = piece.astype(BF16).astype(F32)
    tps[...] = jnp.concatenate([piece] * 4, axis=1)
    tpr[me] = tps[...]
    for dx in range(NX):
        for dc in range(NC):
            if dx or dc:
                remote(
                    tps, tpr.at[me], a_send.at[3], a_recv.at[3],
                    x=xat(dx), c=lax.rem(c + dc, NC),
                ).start()
    x_second(4)
    wait_bytes(zg.at[pl.ds(0, 15)], gzr_sem)
    for dy in range(1, NY):
        remote(zg, yg.at[y], gys_sem, gyr_sem, y=yat(dy)).start()
    for k in range(NZ):
        yg[y, k] = zg[k]
    finish((5, 6))
    finish((0, 1, 2, 3, 4))
    x_second(7)
    x_second(8)
    wait_bytes(tpr.at[pl.ds(0, 7)], a_recv.at[3])
    mixed = tpr[0]
    for k in range(1, NX * NC):
        mixed += tpr[k]
    m_out[...] = mixed[:, :32].astype(BF16)
    wait_bytes(yg.at[pl.ds(0, 3)], gyr_sem)
    field = (iota((16, 128), 1) >> 2) & 3
    gathered = jnp.zeros((16, 128), F32)
    for k in range(NY):
        rows16 = jnp.concatenate([yg[k, i] for i in range(NZ)], axis=0)
        shift = lax.rem(4 * (k - y) + 128, 128)
        gathered += pltpu.roll(jnp.where(field == y, rows16, 0.0), shift, 1)
    spread = jnp.concatenate(
        [jnp.broadcast_to(gathered[k : k + 1, :], (16, 128)) for k in range(NZ)], axis=0
    )
    same = (iota((256, 128), 0) & 15) == (iota((256, 128), 1) & 15)
    spread = jnp.where(same, spread, 0.0)
    pick = (iota((8, 128), 1) >> 4) == iota((8, 128), 0)
    gate_cols = nt_dot(pick.astype(F32), spread, HIGH)
    g_out[0] = gate_cols[0:4]
    g_out[1] = gate_cols[4:8]
    finish((7, 8))
    wait_bytes(sent.at[pl.ds(0, 8)], zs_sem)
    wait_bytes(tbuf.at[0, 0, pl.ds(0, 3)], ys_sem)
    wait_bytes(sent.at[pl.ds(0, 7)], ls_sem)
    wait_bytes(sent.at[pl.ds(0, 7)], rs_sem)
    wait_bytes(tbuf.at[pl.ds(0, 3)], xs_sem)
    wait_bytes(tbuf.at[pl.ds(0, 4)], cs_sem)
    wait_bytes(zg.at[pl.ds(0, 15)], gzs_sem)
    wait_bytes(zg.at[pl.ds(0, 7)], grs_sem)
    wait_bytes(yg.at[pl.ds(0, 3)], gys_sem)
    wait_bytes(az.at[pl.ds(0, 8)], a_send.at[0])
    wait_bytes(far, a_send.at[1])
    wait_bytes(af.at[pl.ds(0, 3)], a_send.at[2])
    wait_bytes(tpr.at[pl.ds(0, 7)], a_send.at[3])


def put_out(*refs):
    ins, outs, sem = refs[:4], refs[4:8], refs[8]
    copies = [
        pltpu.make_async_copy(i, o, sem.at[k]) for k, (i, o) in enumerate(zip(ins, outs))
    ]
    for copy in copies:
        copy.start()
    for copy in copies:
        copy.wait()


def body(tokens, key_weight, value_weight, cum_gate, new_input, new_query, new_gate, out_weight):
    vmem = pl.BlockSpec(memory_space=pltpu.VMEM)
    hbm = pl.BlockSpec(memory_space=pltpu.HBM)
    dma, regular = pltpu.SemaphoreType.DMA, pltpu.SemaphoreType.REGULAR
    shapes = (
        jax.ShapeDtypeStruct((2, 256, 256), BF16),
        jax.ShapeDtypeStruct((2, 256, 256), BF16),
        jax.ShapeDtypeStruct((2, 4, 256), F32),
        jax.ShapeDtypeStruct((2, 32), BF16),
    )
    results = pl.pallas_call(
        kernel,
        out_shape=shapes,
        in_specs=[hbm] * 8,
        out_specs=(vmem,) * 4,
        scratch_shapes=[
            pltpu.VMEM((2, 256, 2048), BF16),
            pltpu.VMEM((2048, 256), BF16),
            pltpu.VMEM((2048, 256), BF16),
            pltpu.VMEM((2, 256, 256), BF16),
            pltpu.VMEM((2, 4, 256), F32),
            pltpu.VMEM((2, 2048), BF16),
            pltpu.VMEM((2, 256), BF16),
            pltpu.VMEM((2, 4), F32),
            pltpu.VMEM((32, 256), BF16),
            pltpu.VMEM((2, 512, 128), F32),
            pltpu.VMEM((NZ, NY, 8, 256), BF16),
            pltpu.VMEM((8, NZ, NY, 8, 256), BF16),
            pltpu.VMEM((2, FAR, NY, 8, 256), BF16),
            pltpu.VMEM((8, 256), F32),
            pltpu.VMEM((NZ, 1, 128), F32),
            pltpu.VMEM((NZ, 1, 128), F32),
            pltpu.VMEM((NY, NZ, 1, 128), F32),
            pltpu.VMEM((8, 1, 128), F32),
            pltpu.VMEM((8, 128), F32),
            pltpu.VMEM((10, 8, 128), F32),
            pltpu.VMEM((2, 8, 128), F32),
            pltpu.VMEM((8, 128), F32),
            pltpu.VMEM((NY, 8, 128), F32),
            pltpu.VMEM((2, 128), F32),
            pltpu.VMEM((8, 2, 128), F32),
            pltpu.VMEM((512, 256), BF16),
            dma((9,)),
            regular((2,)),
            dma, dma, dma, dma, dma, dma,
            dma((9,)), dma((5,)), dma((9,)), dma((9,)),
            dma, dma, dma, dma, dma, dma,
            dma((4,)), dma((4,)),
        ],
        compiler_params=pltpu.CompilerParams(
            collective_id=0, has_side_effects=True, vmem_limit_bytes=24 * 2**20
        ),
    )(
        *(
            pltpu.with_memory_space_constraint(a, pltpu.HBM)
            for a in (
                tokens, key_weight, value_weight, jnp.swapaxes(cum_gate, 1, 2), new_input,
                new_query, new_gate, out_weight.T,
            )
        )
    )
    keys, values, gates, mixed = pl.pallas_call(
        put_out,
        out_shape=shapes,
        in_specs=[vmem] * 4,
        out_specs=(hbm,) * 4,
        scratch_shapes=[dma((4,))],
        compiler_params=pltpu.CompilerParams(vmem_limit_bytes=4 * 2**20),
    )(*results)
    return (
        keys.reshape(2, 1, 256, 256),
        values.reshape(2, 1, 256, 256),
        jnp.swapaxes(gates, 1, 2).reshape(2, 1, 256, 4),
        mixed,
    )


def solution(mesh):
    torus = Mesh(mesh.devices.reshape(NZ, NY, NX, NC), ("z", "y", "x", "c"))
    sp, tp = ("z", "y"), ("x", "c")
    return jax.shard_map(
        body,
        mesh=torus,
        in_specs=(
            P(None, sp, None), P(None, tp), P(None, tp), P(None, sp, tp), P(), P(None, tp),
            P(None, tp), P(tp, sp),
        ),
        out_specs=(P(None, sp, None, tp), P(None, sp, None, tp), P(None, sp, None, tp), P(None, sp)),
        check_vma=False,
    )
```

```python
import jax
import jax.numpy as jnp
from jax import lax
from jax.experimental import pallas as pl
from jax.experimental.pallas import tpu as pltpu
from jax.sharding import Mesh
from jax.sharding import PartitionSpec as P

MESH = pl.DeviceIdType.MESH
F32 = jnp.float32
BF16 = jnp.bfloat16
NZ, NY, NX, NC = 16, 4, 4, 2
HIGH = lax.Precision.HIGHEST
FAR = 4
KV_SLOT = 5


def slots_of(d):
    if d == 0:
        return 0, 1
    if d == NZ // 2:
        return NZ - 1, 1
    return 2 * d - 1, 2


def iota(shape, dim):
    return lax.broadcasted_iota(jnp.int32, shape, dim)


def nt_dot(a, b, precision=None):
    return lax.dot_general(
        a, b, (((1,), (1,)), ((), ())), precision=precision, preferred_element_type=F32
    )


def fold_heads(wide):
    half = wide[:, :128] + wide[:, 128:]
    return half + pltpu.roll(half, 64, 1)


def merge(parts):
    tops = [p[:, 65:66] for p in parts]
    top = tops[0]
    for t in tops[1:]:
        top = jnp.maximum(top, t)
    total = None
    for p, t in zip(parts, tops):
        term = p * jnp.exp(t - top)
        total = term if total is None else total + term
    lane = iota(total.shape, 1)
    return jnp.where(lane == 65, top, total)


def kernel(
    tok_hbm, wk_hbm, wv_hbm, gate_hbm, new_in_hbm, query_hbm, new_gate_hbm, ow_hbm,
    k_out, v_out, g_out, m_out,
    tok, wk, wv, part, gate_ref, new_in_ref, query_ref, new_gate_ref, ow_ref,
    order, sent, sent_kv, kv_in, tbuf, relay, g8, pg, zg, yg, grelay, azs, az, far, afs, af, tps, tpr, kv_loc,
    sem_in, d_sem, zs_sem, ks_sem, ys_sem, ls_sem, rs_sem, xs_sem, cs_sem, zr_sem, lr_sem, xr_sem, cr_sem,
    gzs_sem, gzr_sem, grs_sem, grr_sem, gys_sem, gyr_sem, a_send, a_recv,
):
    z, y = lax.axis_index("z"), lax.axis_index("y")
    x, c = lax.axis_index("x"), lax.axis_index("c")
    me = x * NC + c

    def zat(d):
        return lax.rem(z + (d + NZ), NZ)

    def yat(d):
        return lax.rem(y + d, NY)

    def xat(d):
        return lax.rem(x + (d + NX), NX)

    def remote(src, dst, ssem, rsem, **dev):
        return pltpu.make_async_remote_copy(
            src_ref=src, dst_ref=dst, send_sem=ssem, recv_sem=rsem,
            device_id=dev, device_id_type=MESH,
        )

    def wait_bytes(ref, sem):
        pltpu.make_async_copy(ref, ref, sem).wait()

    def signal(sem, **dev):
        pl.semaphore_signal(sem, inc=1, device_id=dev, device_id_type=MESH)

    barrier = pltpu.get_barrier_semaphore()
    cols = pl.ds(pl.multiple_of(me * 256, 256), 256)
    sources = (
        (tok_hbm.at[:, :, cols], part), (tok_hbm, tok), (wk_hbm, wk), (wv_hbm, wv),
        (gate_hbm, gate_ref), (new_in_hbm, new_in_ref), (query_hbm, query_ref),
        (new_gate_hbm, new_gate_ref), (ow_hbm, ow_ref),
    )
    loads = [pltpu.make_async_copy(s, d, sem_in.at[k]) for k, (s, d) in enumerate(sources)]
    load_part, load_tok, load_wk, load_wv, load_gate, load_in, load_q, load_ng, load_ow = loads
    load_part.start()
    for dz in (1, -1):
        for dy in range(NY):
            signal(barrier, z=zat(dz), y=yat(dy))
    for dy in range(1, NY):
        signal(barrier, y=yat(dy))
    for dx in range(NX):
        for dc in range(NC):
            if dx or dc:
                signal(barrier, x=xat(dx), c=lax.rem(c + dc, NC))
    for load in (load_gate, load_q, load_ng, load_in, load_wk, load_tok, load_wv, load_ow):
        load.start()

    def slot_at(d, sign):
        first, count = slots_of(d)
        return first + 1 if sign > 0 and count == 2 else first

    def send_z(d):
        for sign in (1, -1):
            to = zat(sign * d)
            for dy in range(NY):
                remote(
                    sent.at[to, yat(dy)], tbuf.at[me, slot_at(d, sign), y], zs_sem, zr_sem.at[d],
                    z=to, y=yat(dy),
                ).start()

    def send_kv(d):
        for sign in (1, -1):
            to = zat(sign * d)
            for dy in range(NY):
                for q in range(2):
                    remote(
                        sent_kv.at[q, to, yat(dy)], kv_in.at[q, slot_at(d, sign) - KV_SLOT, y],
                        ks_sem, zr_sem.at[d], z=to, y=yat(dy),
                    ).start()

    def to_relay(k):
        for way, sign in enumerate((1, -1)):
            to = zat(sign * (FAR + k))
            if k < FAR:
                src, dst = sent.at[to], relay.at[way, k - 1]
            else:
                src, dst = sent.at[to, pl.ds(2 * way, 2)], relay.at[way, k - 1, pl.ds(0, 2)]
            remote(src, dst, ls_sem, lr_sem.at[k], z=zat(sign * FAR)).start()

    def pass_on(k):
        came = relay.at[:, k - 1] if k < FAR else relay.at[:, k - 1, pl.ds(0, 2)]
        wait_bytes(came, lr_sem.at[k])
        for way, sign in enumerate((1, -1)):
            for q in range(NY if k < FAR else 2):
                remote(
                    relay.at[way, k - 1, q], tbuf.at[me, slot_at(FAR + k, sign), y], rs_sem,
                    zr_sem.at[FAR + k], z=zat(sign * k), y=q if k < FAR else q + 2 * way,
                ).start()

    def slots(d):
        first, count = slots_of(d)
        return pl.ds(first, count)

    def x_first(d):
        here = tbuf.at[me, slots(d)]
        if d:
            wait_bytes(here, zr_sem.at[d])
        else:
            wait_bytes(tbuf.at[me, 0, pl.ds(0, 3)], zr_sem.at[0])
        for dx in (1, -1, 2):
            remote(here, here, xs_sem, xr_sem.at[d], x=xat(dx)).start()
        remote(here, here, cs_sem, cr_sem.at[d], c=1 - c).start()

    def x_second(d):
        wait_bytes(tbuf.at[pl.ds(0, 3), slots(d)], xr_sem.at[d])
        for dx in range(1, NX):
            came = tbuf.at[xat(dx) * NC + c, slots(d)]
            remote(came, came, cs_sem, cr_sem.at[d], c=1 - c).start()

    def lay_out(rows, out, first, count):
        rows = rows.reshape(count * 2, 2, 8, 256)
        even, odd = rows[:, 0], rows[:, 1]
        low = iota(even.shape, 1) < 4
        for b, (a0, a1) in enumerate(
            ((even, pltpu.roll(odd, 4, 1)), (pltpu.roll(even, 4, 1), odd))
        ):
            block = jnp.where(low, a0, a1).reshape(count, 16, 256).astype(BF16)
            for k in range(count):
                slot = first + k
                rel = 0 if slot == 0 else 8 if slot == NZ - 1 else (
                    (slot + 1) // 2 if slot % 2 else -(slot // 2)
                )
                at = pl.multiple_of(zat(rel) * 16, 16)
                out[b, pl.ds(at, 16), :] = block[k]

    def place(d):
        first, count = slots_of(d)
        came = pl.ds(first - KV_SLOT, count)
        wait_bytes(kv_in.at[:, came], zr_sem.at[d])
        for q, out in enumerate((k_out, v_out)):
            lay_out(kv_in[q, came].astype(F32), out, first, count)

    def finish(ds):
        for d in ds:
            wait_bytes(tbuf.at[pl.ds(0, 4), slots(d)], cr_sem.at[d])
        first = min(slots_of(d)[0] for d in ds)
        count = sum(slots_of(d)[1] for d in ds)
        for w, out in ((wk, k_out), (wv, v_out)):
            acc = None
            for f in range(8):
                lhs = tbuf[f, first : first + count].reshape(count * NY, 8, 256)
                lhs = lhs.astype(F32).reshape(count * 32, 256).astype(BF16)
                term = jnp.dot(
                    lhs, w[f * 256 : (f + 1) * 256, :], preferred_element_type=F32
                )
                acc = term if acc is None else acc + term
            lay_out(acc, out, first, count)

    pl.semaphore_wait(barrier, 3 + 7 + 8)
    for s in (1, -1):
        signal(d_sem.at[0], z=zat(s))
    load_part.wait()
    def rows_by_peer(rows, dst):
        for k in range(2):
            for b in range(2):
                for j in range(4):
                    order[k, pl.ds(4 * b + j, 64, stride=8), :] = rows(256 * b + 64 * j, k).astype(F32)
            dst[:, :, :, 128 * k : 128 * k + 128] = order[k].reshape(NZ, NY, 8, 128).astype(BF16)

    rows_by_peer(
        lambda lo, k: part[lo // 256, lo % 256 : lo % 256 + 64, 128 * k : 128 * k + 128], sent
    )
    for dy in range(1, NY):
        remote(
            sent.at[z, yat(dy)], tbuf.at[me, 0, y], ys_sem, zr_sem.at[0], y=yat(dy)
        ).start()
    send_z(1)
    tbuf[me, 0, y] = sent[z, y]
    pl.semaphore_wait(d_sem.at[0], 2)
    for s in (2, -2):
        signal(d_sem.at[1], z=zat(s))
    send_z(2)

    head_of_row = iota((8, 256), 0) & 3
    mine = (iota((8, 256), 1) >> 6) == head_of_row
    second = iota((8, 256), 0) >= 4

    def by_row(two):
        return jnp.where(
            second, jnp.broadcast_to(two[1:2, :], (8, 256)), jnp.broadcast_to(two[0:1, :], (8, 256))
        )

    for load in (load_q, load_ng, load_in):
        load.wait()
    query = jnp.where(mine, by_row(query_ref[...].astype(F32)), 0.0)
    query_b = query.astype(BF16)
    new_in = new_in_ref[...]
    load_gate.wait()
    g8[0:4, :] = gate_ref[0]
    g8[4:8, :] = gate_ref[1]
    gates = g8[...]
    lanes, rows = iota((128, 256), 1), iota((128, 256), 0)
    spread = jnp.concatenate(
        [jnp.broadcast_to(gates[k : k + 1, :], (16, 256)) for k in range(8)], axis=0
    )
    same = ((lanes & 3) == ((rows >> 2) & 3)) & ((lanes >> 6) == (rows & 3))
    spread = jnp.where(same, spread, 0.0)
    pick = ((iota((16, 256), 1) >> 2) & 15) == iota((16, 256), 0)
    gate_rows = nt_dot(pick.astype(F32), spread, HIGH)
    for k in range(NZ):
        pg[k] = gate_rows[k : k + 1, :]

    pl.semaphore_wait(d_sem.at[1], 2)
    to_relay(4)
    to_relay(1)
    to_relay(3)
    load_wk.wait()
    load_tok.wait()
    key_now = jnp.dot(new_in, wk[...], preferred_element_type=F32).astype(BF16).astype(F32)
    local = tok[...].reshape(512, 2048)
    kv_loc[0] = jnp.dot(local, wk[...], preferred_element_type=F32).astype(BF16)
    raw = jnp.where(
        second, nt_dot(query_b, kv_loc[0, 256:]), nt_dot(query_b, kv_loc[0, :256])
    )
    ng = new_gate_ref[...]
    ng = jnp.where(
        iota((8, 4), 0) >= 4,
        jnp.broadcast_to(ng[1:2, :], (8, 4)),
        jnp.broadcast_to(ng[0:1, :], (8, 4)),
    )
    ng = jnp.sum(
        jnp.where((iota((8, 4), 0) & 3) == iota((8, 4), 1), ng, 0.0), axis=1, keepdims=True
    )
    scores = raw * 0.125 + ng - g8[...]
    top = jnp.max(scores, axis=1, keepdims=True)
    expo = jnp.exp(scores - top)
    total = jnp.sum(expo, axis=1, keepdims=True)
    expo_b = expo.astype(BF16)
    x_first(0)
    load_wv.wait()
    kv_loc[1] = jnp.dot(local, wv[...], preferred_element_type=F32).astype(BF16)
    x_first(1)
    x_first(2)
    num = jnp.where(
        second,
        jnp.dot(expo_b, kv_loc[1, 256:], preferred_element_type=F32),
        jnp.dot(expo_b, kv_loc[1, :256], preferred_element_type=F32),
    )
    num = fold_heads(jnp.where(mine, num, 0.0))
    lane = iota((8, 128), 1)
    packed = jnp.where(
        lane < 64, num, jnp.where(lane == 64, total, jnp.where(lane == 65, top, 0.0))
    )
    azs[...] = packed
    for d in range(1, FAR + 1):
        for sign in (1, -1):
            slot = d - 1 if sign < 0 else FAR + d - 1
            remote(azs, az.at[slot], a_send.at[0], a_recv.at[0], z=zat(sign * d)).start()
    zg[z] = pg[z]
    for sign in (1, -1):
        for d in range(1, FAR + 1):
            remote(pg.at[zat(sign * d)], zg.at[z], gzs_sem, gzr_sem, z=zat(sign * d)).start()
    for way, sign in enumerate((1, -1)):
        for k in range(1, FAR + 1 - way):
            remote(
                pg.at[zat(sign * (FAR + k))], grelay.at[FAR * way + k - 1], gzs_sem, grr_sem,
                z=zat(sign * FAR),
            ).start()
    to_relay(2)
    pass_on(1)
    x_second(0)
    for q in range(2):
        rows_by_peer(lambda lo, k: kv_loc[q, lo : lo + 64, 128 * k : 128 * k + 128], sent_kv.at[q])
    pass_on(3)
    pass_on(4)
    x_second(1)
    value_now = jnp.dot(new_in, wv[...], preferred_element_type=F32).astype(BF16).astype(F32)
    wait_bytes(az.at[pl.ds(0, 8)], a_recv.at[0])
    far[0] = merge([az[k] for k in range(FAR)])
    far[1] = merge([az[k] for k in range(FAR, 2 * FAR - 1)])
    remote(far.at[0], az.at[8], a_send.at[1], a_recv.at[1], z=zat(-FAR)).start()
    remote(far.at[1], az.at[9], a_send.at[1], a_recv.at[1], z=zat(FAR)).start()
    x_second(2)
    wait_bytes(zg.at[pl.ds(0, 7)], grr_sem)
    for way, sign in enumerate((1, -1)):
        for k in range(1, FAR + 1 - way):
            remote(
                grelay.at[FAR * way + k - 1], zg.at[zat(-sign * FAR)], grs_sem, gzr_sem,
                z=zat(sign * k),
            ).start()
    pass_on(2)
    x_first(5)
    x_first(7)
    send_kv(4)
    wait_bytes(zg.at[pl.ds(0, 15)], gzr_sem)
    for dy in range(1, NY):
        remote(zg, yg.at[y], gys_sem, gyr_sem, y=yat(dy)).start()
    for k in range(NZ):
        yg[y, k] = zg[k]
    x_first(8)
    wait_bytes(az.at[pl.ds(8, 2)], a_recv.at[1])
    merged = merge([azs[...]] + [az[k] for k in range(10)])
    afs[...] = merged
    af[y] = merged
    for dy in range(1, NY):
        remote(afs, af.at[y], a_send.at[2], a_recv.at[2], y=yat(dy)).start()
    send_kv(3)
    x_first(6)
    x_second(7)
    load_ow.wait()
    wait_bytes(af.at[pl.ds(0, 3)], a_recv.at[2])
    cached = merge([af[k] for k in range(NY)])
    own = jnp.sum(query * by_row(key_now), axis=1, keepdims=True) * 0.125
    cached_top, cached_total = cached[:, 65:66], cached[:, 64:65]
    cached_num = jnp.where(lane < 64, cached, pltpu.roll(cached, 64, 1))
    highest = jnp.maximum(cached_top, own)
    keep = jnp.exp(cached_top - highest)
    own_expo = jnp.exp(own - highest)
    totals = cached_total * keep + own_expo
    value_rows = fold_heads(jnp.where(mine, by_row(value_now), 0.0))
    numer = cached_num * keep + own_expo.astype(BF16).astype(F32) * value_rows
    attended = (numer / totals).astype(BF16).astype(F32)
    attended = jnp.where(mine, jnp.concatenate([attended, attended], axis=1), 0.0).astype(BF16)
    piece = nt_dot(attended, ow_ref[...])
    piece = jnp.concatenate(
        [jnp.sum(piece[0:4], axis=0, keepdims=True), jnp.sum(piece[4:8], axis=0, keepdims=True)],
        axis=0,
    )
    piece = piece.astype(BF16).astype(F32)
    tps[...] = jnp.concatenate([piece] * 4, axis=1)
    tpr[me] = tps[...]
    for dx in range(NX):
        for dc in range(NC):
            if dx or dc:
                remote(
                    tps, tpr.at[me], a_send.at[3], a_recv.at[3],
                    x=xat(dx), c=lax.rem(c + dc, NC),
                ).start()
    x_second(8)
    wait_bytes(yg.at[pl.ds(0, 3)], gyr_sem)
    field = (iota((16, 128), 1) >> 2) & 3
    gathered = jnp.zeros((16, 128), F32)
    for k in range(NY):
        rows16 = jnp.concatenate([yg[k, i] for i in range(NZ)], axis=0)
        shift = lax.rem(4 * (k - y) + 128, 128)
        gathered += pltpu.roll(jnp.where(field == y, rows16, 0.0), shift, 1)
    spread = jnp.concatenate(
        [jnp.broadcast_to(gathered[k : k + 1, :], (16, 128)) for k in range(NZ)], axis=0
    )
    same = (iota((256, 128), 0) & 15) == (iota((256, 128), 1) & 15)
    spread = jnp.where(same, spread, 0.0)
    pick = (iota((8, 128), 1) >> 4) == iota((8, 128), 0)
    gate_cols = nt_dot(pick.astype(F32), spread, HIGH)
    g_out[0] = gate_cols[0:4]
    g_out[1] = gate_cols[4:8]
    x_second(5)
    x_second(6)
    finish((0, 1, 2))
    place(4)
    finish((7, 8))
    place(3)
    finish((5, 6))
    wait_bytes(tpr.at[pl.ds(0, 7)], a_recv.at[3])
    mixed = tpr[0]
    for k in range(1, NX * NC):
        mixed += tpr[k]
    m_out[...] = mixed[:, :32].astype(BF16)
    wait_bytes(sent.at[pl.ds(0, 4)], zs_sem)
    wait_bytes(sent.at[pl.ds(0, 8)], ks_sem)
    wait_bytes(tbuf.at[0, 0, pl.ds(0, 3)], ys_sem)
    wait_bytes(sent.at[pl.ds(0, 7)], ls_sem)
    wait_bytes(sent.at[pl.ds(0, 7)], rs_sem)
    wait_bytes(tbuf.at[pl.ds(0, 3), pl.ds(0, 12)], xs_sem)
    wait_bytes(tbuf.at[pl.ds(0, 4), pl.ds(0, 12)], cs_sem)
    wait_bytes(zg.at[pl.ds(0, 15)], gzs_sem)
    wait_bytes(zg.at[pl.ds(0, 7)], grs_sem)
    wait_bytes(yg.at[pl.ds(0, 3)], gys_sem)
    wait_bytes(az.at[pl.ds(0, 8)], a_send.at[0])
    wait_bytes(far, a_send.at[1])
    wait_bytes(af.at[pl.ds(0, 3)], a_send.at[2])
    wait_bytes(tpr.at[pl.ds(0, 7)], a_send.at[3])


def put_out(*refs):
    ins, outs, sem = refs[:4], refs[4:8], refs[8]
    copies = [
        pltpu.make_async_copy(i, o, sem.at[k]) for k, (i, o) in enumerate(zip(ins, outs))
    ]
    for copy in copies:
        copy.start()
    for copy in copies:
        copy.wait()


def body(tokens, key_weight, value_weight, cum_gate, new_input, new_query, new_gate, out_weight):
    vmem = pl.BlockSpec(memory_space=pltpu.VMEM)
    hbm = pl.BlockSpec(memory_space=pltpu.HBM)
    dma, regular = pltpu.SemaphoreType.DMA, pltpu.SemaphoreType.REGULAR
    shapes = (
        jax.ShapeDtypeStruct((2, 256, 256), BF16),
        jax.ShapeDtypeStruct((2, 256, 256), BF16),
        jax.ShapeDtypeStruct((2, 4, 256), F32),
        jax.ShapeDtypeStruct((2, 32), BF16),
    )
    results = pl.pallas_call(
        kernel,
        out_shape=shapes,
        in_specs=[hbm] * 8,
        out_specs=(vmem,) * 4,
        scratch_shapes=[
            pltpu.VMEM((2, 256, 2048), BF16),
            pltpu.VMEM((2048, 256), BF16),
            pltpu.VMEM((2048, 256), BF16),
            pltpu.VMEM((2, 256, 256), BF16),
            pltpu.VMEM((2, 4, 256), F32),
            pltpu.VMEM((2, 2048), BF16),
            pltpu.VMEM((2, 256), BF16),
            pltpu.VMEM((2, 4), F32),
            pltpu.VMEM((32, 256), BF16),
            pltpu.VMEM((2, 512, 128), F32),
            pltpu.VMEM((NZ, NY, 8, 256), BF16),
            pltpu.VMEM((2, NZ, NY, 8, 256), BF16),
            pltpu.VMEM((2, 4, NY, 8, 256), BF16),
            pltpu.VMEM((8, NZ, NY, 8, 256), BF16),
            pltpu.VMEM((2, FAR, NY, 8, 256), BF16),
            pltpu.VMEM((8, 256), F32),
            pltpu.VMEM((NZ, 1, 128), F32),
            pltpu.VMEM((NZ, 1, 128), F32),
            pltpu.VMEM((NY, NZ, 1, 128), F32),
            pltpu.VMEM((8, 1, 128), F32),
            pltpu.VMEM((8, 128), F32),
            pltpu.VMEM((10, 8, 128), F32),
            pltpu.VMEM((2, 8, 128), F32),
            pltpu.VMEM((8, 128), F32),
            pltpu.VMEM((NY, 8, 128), F32),
            pltpu.VMEM((2, 128), F32),
            pltpu.VMEM((8, 2, 128), F32),
            pltpu.VMEM((2, 512, 256), BF16),
            dma((9,)),
            regular((2,)),
            dma, dma, dma, dma, dma, dma, dma,
            dma((9,)), dma((5,)), dma((9,)), dma((9,)),
            dma, dma, dma, dma, dma, dma,
            dma((4,)), dma((4,)),
        ],
        compiler_params=pltpu.CompilerParams(
            collective_id=0, has_side_effects=True, vmem_limit_bytes=24 * 2**20
        ),
    )(
        *(
            pltpu.with_memory_space_constraint(a, pltpu.HBM)
            for a in (
                tokens, key_weight, value_weight, jnp.swapaxes(cum_gate, 1, 2), new_input,
                new_query, new_gate, out_weight.T,
            )
        )
    )
    keys, values, gates, mixed = pl.pallas_call(
        put_out,
        out_shape=shapes,
        in_specs=[vmem] * 4,
        out_specs=(hbm,) * 4,
        scratch_shapes=[dma((4,))],
        compiler_params=pltpu.CompilerParams(vmem_limit_bytes=4 * 2**20),
    )(*results)
    return (
        keys.reshape(2, 1, 256, 256),
        values.reshape(2, 1, 256, 256),
        jnp.swapaxes(gates, 1, 2).reshape(2, 1, 256, 4),
        mixed,
    )


def solution(mesh):
    torus = Mesh(mesh.devices.reshape(NZ, NY, NX, NC), ("z", "y", "x", "c"))
    sp, tp = ("z", "y"), ("x", "c")
    return jax.shard_map(
        body,
        mesh=torus,
        in_specs=(
            P(None, sp, None), P(None, tp), P(None, tp), P(None, sp, tp), P(), P(None, tp),
            P(None, tp), P(tp, sp),
        ),
        out_specs=(P(None, sp, None, tp), P(None, sp, None, tp), P(None, sp, None, tp), P(None, sp)),
        check_vma=False,
    )
```
